512 devices in a mesh: sp: 64 (over z, y), tp: 8 (over x, core).
Axes of the slice: x: 4, y: 4, z: 16, core: 2. Of those that a mesh axis runs over, the one named last changes fastest.
Arguments:
- tokens: bfloat16 [8192, 1024], P('sp', 'tp'), may hold values from -6 to 6
- norm_gain: float32 [1024], P('tp'), may hold values from 0.1 to 1.9
- query_weight: bfloat16 [1024, 1024], P('sp', 'tp'), may hold values from -0.1875 to 0.1875
- key_weight: bfloat16 [1024, 512], P('sp', 'tp'), may hold values from -0.1875 to 0.1875
- value_weight: bfloat16 [1024, 512], P('sp', 'tp'), may hold values from -0.1875 to 0.1875
- conv_in_weight: bfloat16 [1024, 1024], P('sp', 'tp'), may hold values from -0.1875 to 0.1875
- pre_weight: bfloat16 [1024, 1024], P('sp', 'tp'), may hold values from -0.1875 to 0.1875
- post_weight: bfloat16 [1024, 1024], P('sp', 'tp'), may hold values from -0.1875 to 0.1875
- attn_gate_weight: bfloat16 [1024, 1024], P('sp', 'tp'), may hold values from -0.1875 to 0.1875
- conv_gate_weight: bfloat16 [1024, 1024], P('sp', 'tp'), may hold values from -0.1875 to 0.1875
- sink_logit: float32 [16], P('tp'), may hold values from 1 to 5
- conv_taps: float32 [3, 1024], P(None, 'tp'), may hold values from -3 to 3
- attn_out_weight: bfloat16 [1024, 1024], P('tp', 'sp'), may hold values from -1 to 1
- conv_out_weight: bfloat16 [1024, 1024], P('tp', 'sp'), may hold values from -0.1875 to 0.1875
Outputs:
- merged: bfloat16 [8192, 1024], P('sp', 'tp')
The draws below stay inside these ranges and needn't reach their ends.
All inputs are finite; a program needn't handle non-finite values.
Results may differ from the reference program's by a relative error of at most 0.003.
Values may be sent and summed in bfloat16 or wider, within the bound.
A program may use at most 64 MiB of HBM per device.

```python
import jax
import jax.numpy as jnp
from jax import lax

D = 1024
Q_HEADS = 16
KV_HEADS = 8
HEAD_DIM = 64
WINDOW = 64
TOK_DEV = 128
GROUP = 2
ATTN_WIDTH = 1024
KV_WIDTH = 512
TOKENS = 8192


def steps_of(rng, extent, pieces, low, top_value):
    level, own = 1.0, jax.random.fold_in(rng, 6)
    for position, parts in pieces:
        heights = jnp.exp(jax.random.uniform(jax.random.fold_in(own, position), (parts,), jnp.float32, low / len(pieces), top_value / len(pieces)))
        level = level * jnp.repeat(heights, extent[position] // parts).reshape([-1 if axis == position else 1 for axis in range(len(extent))])
    return level


def centred(rng, shape, width, limit, shards=(), kind=jnp.bfloat16):
    result = jax.random.normal(rng, shape, jnp.float32) * width
    if len(shards) > 0:
        result = steps_of(rng, shape, shards, -0.22, 0.18) * result
    return jnp.clip(result, min=-limit, max=limit).astype(kind)


def setup_inputs(seed: int = 0) -> dict:
    arg_keys = jax.random.split(jax.random.key(seed), 15)
    return {
        "tokens": centred(arg_keys[0], (TOKENS, D), 1.0, 6.0, ((0, 64), (1, 8))),
        "norm_gain": jnp.clip(1.0 + 0.18 * jax.random.normal(arg_keys[1], (D,), jnp.float32), 0.1, 1.9),
        "query_weight": centred(arg_keys[2], (D, ATTN_WIDTH), D ** -0.5, 0.1875, ((0, 64), (1, 8))),
        "key_weight": centred(arg_keys[3], (D, KV_WIDTH), D ** -0.5, 0.1875, ((0, 64), (1, 8))),
        "value_weight": centred(arg_keys[4], (D, KV_WIDTH), D ** -0.5, 0.1875, ((0, 64), (1, 8))),
        "conv_in_weight": centred(arg_keys[5], (D, D), D ** -0.5, 0.1875, ((0, 64), (1, 8))),
        "pre_weight": centred(arg_keys[6], (D, D), D ** -0.5, 0.1875, ((0, 64), (1, 8))),
        "post_weight": centred(arg_keys[7], (D, D), D ** -0.5, 0.1875, ((0, 64), (1, 8))),
        "attn_gate_weight": centred(arg_keys[8], (D, D), D ** -0.5, 0.1875, ((0, 64), (1, 8))),
        "conv_gate_weight": centred(arg_keys[9], (D, D), D ** -0.5, 0.1875, ((0, 64), (1, 8))),
        "sink_logit": jnp.clip(1.0 + 4.0 * jax.random.uniform(arg_keys[10], (Q_HEADS,), jnp.float32) ** steps_of(arg_keys[10], (Q_HEADS,), ((0, 8),), -0.2, 0.2), 1.0, 5.0),
        "conv_taps": centred(arg_keys[11], (3, D), 0.577, 3.0, ((1, 8),), jnp.float32),
        "attn_out_weight": centred(arg_keys[12], (ATTN_WIDTH, D), (ATTN_WIDTH // 32) ** -0.5, 1.0, ((0, 8), (1, 64))),
        "conv_out_weight": centred(arg_keys[13], (D, D), D ** -0.5, 0.1875, ((0, 8), (1, 64))),
    }


epsilon = 1e-06
negative = -1e+30

def window_mix(queries, key_rows, value_rows, sink_cols, first, seq_total):
    score_scale = queries.shape[-1] ** (-0.5)
    scores = jnp.einsum('qhgd,khd->hgqk', queries, key_rows, precision=lax.Precision.HIGHEST) * score_scale
    qpos = first + jnp.arange(queries.shape[0], dtype=jnp.int32)
    kpos = first - WINDOW + jnp.arange(key_rows.shape[0], dtype=jnp.int32)
    allowed = (jnp.abs(qpos[:, None] - kpos[None, :]) <= WINDOW) & (kpos >= 0)[None, :] & (kpos < seq_total)[None, :]
    scores = jnp.where(allowed, scores, negative)
    column = jnp.broadcast_to(sink_cols[:, :, None, None], scores.shape[:-1] + (1,))
    weights_soft = jax.nn.softmax(jnp.concatenate([scores, column], axis=-1), axis=-1)[..., :-1]
    return jnp.einsum('hgqk,khd->qhgd', weights_soft, value_rows, precision=lax.Precision.HIGHEST)

def attention(queries, key_rows, value_rows, sink_logit):
    padding = ((WINDOW, WINDOW), (0, 0))
    key_pad = jnp.pad(key_rows.astype(jnp.float32), padding)
    value_pad = jnp.pad(value_rows.astype(jnp.float32), padding)
    span_rows = TOK_DEV + 2 * WINDOW
    sink_cols = sink_logit.reshape(KV_HEADS, GROUP)

    def block(block_index):
        first = block_index * TOK_DEV
        q_block = lax.dynamic_slice_in_dim(queries, first, TOK_DEV, 0).astype(jnp.float32)
        q_block = q_block.reshape(TOK_DEV, KV_HEADS, GROUP, HEAD_DIM)
        k_block = lax.dynamic_slice_in_dim(key_pad, first, span_rows, 0).reshape(span_rows, KV_HEADS, HEAD_DIM)
        v_block = lax.dynamic_slice_in_dim(value_pad, first, span_rows, 0).reshape(span_rows, KV_HEADS, HEAD_DIM)
        mixed_rows = window_mix(q_block, k_block, v_block, sink_cols, first, TOKENS)
        return mixed_rows.reshape(TOK_DEV, ATTN_WIDTH)
    blocks_out = lax.map(block, jnp.arange(TOKENS // TOK_DEV, dtype=jnp.int32))
    return blocks_out.reshape(TOKENS, ATTN_WIDTH).astype(jnp.bfloat16)

def reference(tokens, norm_gain, query_weight, key_weight, value_weight, conv_in_weight, pre_weight, post_weight, attn_gate_weight, conv_gate_weight, sink_logit, conv_taps, attn_out_weight, conv_out_weight):
    widened = tokens.astype(jnp.float32)
    mean_sq = lax.optimization_barrier(jnp.mean(widened * widened, axis=1, keepdims=True))
    normed = (widened * lax.rsqrt(mean_sq + epsilon) * norm_gain[None, :]).astype(jnp.bfloat16)

    def project(weight):
        return jnp.dot(normed, weight, preferred_element_type=jnp.float32)
    queries = project(query_weight).astype(jnp.bfloat16)
    key_rows = project(key_weight).astype(jnp.bfloat16)
    value_rows = project(value_weight).astype(jnp.bfloat16)
    conv_in = project(conv_in_weight).astype(jnp.bfloat16)
    pre_gate = project(pre_weight).astype(jnp.bfloat16)
    post_gate = project(post_weight).astype(jnp.bfloat16)
    attn_gate = project(attn_gate_weight)
    conv_gate = project(conv_gate_weight)
    attended = attention(queries, key_rows, value_rows, sink_logit)
    conv_mix = (pre_gate.astype(jnp.float32) * conv_in.astype(jnp.float32)).astype(jnp.bfloat16)
    padded = jnp.pad(conv_mix.astype(jnp.float32), ((1, 1), (0, 0)))
    convolved = conv_taps[0][None, :] * padded[:-2] + conv_taps[1][None, :] * padded[1:-1] + conv_taps[2][None, :] * padded[2:]
    conv_out = (post_gate.astype(jnp.float32) * convolved).astype(jnp.bfloat16)
    branch_attn = jnp.dot(attended, attn_out_weight, preferred_element_type=jnp.float32)
    branch_conv = jnp.dot(conv_out, conv_out_weight, preferred_element_type=jnp.float32)
    return (jax.nn.sigmoid(attn_gate) * branch_attn + jax.nn.sigmoid(conv_gate) * branch_conv).astype(jnp.bfloat16)
```

```python
import jax
import jax.numpy as jnp
from jax import lax
from jax.experimental import pallas as pl
from jax.experimental.pallas import tpu as pltpu
from jax.sharding import Mesh
from jax.sharding import PartitionSpec as P

MESH = pl.DeviceIdType.MESH
NZ, NY, NX = 16, 4, 4
TOK = 128
ROWS = NY * TOK
HALO = 64
SEQ = NZ * ROWS
EPS = 1e-06
NEG = -1e30
F32 = jnp.float32
BF16 = jnp.bfloat16


def lanes(shape):
    return lax.broadcasted_iota(jnp.int32, shape, len(shape) - 1)


def swap(v):
    return pltpu.roll(v, 64, v.ndim - 1)


def fold(v):
    low, high = v[: v.shape[0] // 2], v[v.shape[0] // 2 :]
    return jnp.where(lanes(low.shape) < 64, swap(low), high)


def unfold(a, b):
    first = lanes(a.shape) < 64
    return jnp.where(first, a, swap(b)), jnp.where(first, swap(a), b)


def kernel(
    tokens, gain, wq, wk, wv, wci, wpre, wpost, wag, wcg, sink, taps, wao, wco,
    out,
    tok, par, w, ow, normed, kv, qp, gsend, grecv, asend, arecv, left, xsend, xrecv,
    raw, rawk, rawv, rawo, rawg, rawt, raws, pack, opack,
    load_sem, a_send, a_recv, t_send, tx_recv, ty_recv, td_recv, p_send, px_recv, pd_recv,
    w_send, w_recv, o1_send, o1_recv, o2_send, o2_recv, o3_send, o3_recv,
    h_send, h_recv, g_send, g_recv, e_send, e_recv, d_send, d_recv,
):
    z, y, x, c = (lax.axis_index(n) for n in ("z", "y", "x", "c"))

    def at(dz=0, ny=None, nx=None, nc=None):
        return (
            lax.rem(z + dz + NZ, NZ) if dz else z,
            y if ny is None else ny,
            x if nx is None else nx,
            c if nc is None else nc,
        )

    ys = [lax.rem(y + d, NY) for d in (1, 2, 3)]
    xs = [lax.rem(x + d, NX) for d in (1, 2, 3)]
    other = 1 - c

    barrier = pltpu.get_barrier_semaphore()
    peers = [at(dz=d) for d in (-2, -1, 1, 2)] + [at(nc=other)]
    peers += [at(ny=n, nc=m) for n in ys for m in (c, other)]
    peers += [at(nx=n, nc=m) for n in xs for m in (c, other)]
    for peer in peers:
        pl.semaphore_signal(barrier, inc=1, device_id=peer, device_id_type=MESH)

    loads = []

    def load(src, dst):
        copy = pltpu.make_async_copy(src, dst, load_sem.at[len(loads)])
        copy.start()
        loads.append(copy)

    for k, ref in enumerate((wq, wag, wci, wcg, wpre, wpost)):
        load(ref, raw.at[k])
    load(wk, rawk)
    load(wv, rawv)
    load(gain, rawg)
    load(taps, rawt)
    load(sink, raws)
    load(tokens, tok.at[y, c, x])
    load(wao, rawo.at[0])
    load(wco, rawo.at[1])
    for copy in loads:
        copy.wait()

    q32, ag32, ci32, cg32, pre32, post32 = (raw[k].astype(F32) for k in range(6))
    first = lanes((16, 128)) < 64
    kv32 = jnp.concatenate([rawk[...].astype(F32), rawv[...].astype(F32)], axis=1)

    def joined(a, b, half):
        return jnp.where(first, a, swap(b)) if half == 0 else jnp.where(first, swap(a), b)

    for b in range(2):
        pack[b, 0, :, :128] = joined(q32, ag32, b).astype(BF16)
        pack[b, 0, :, 128:] = kv32.astype(BF16)
        pack[b, 1, :, :128] = joined(ci32, cg32, b).astype(BF16)
        pack[b, 1, :, 128:] = joined(pre32, post32, b).astype(BF16)
    for m in range(2):
        opack[m] = rawo[m].astype(F32).T.astype(BF16)
    par[c, x] = jnp.zeros((8, 128), F32)
    par[c, x, 0:1, :] = rawg[...]
    par[c, x, 1:4, :] = rawt[...]
    par[c, x, 4:5, 0:2] = raws[...]

    pl.semaphore_wait(barrier, len(peers))

    ends = []

    def send(src, dst, send_sem, recv_sem, device, when=None):
        copy = pltpu.make_async_remote_copy(
            src_ref=src, dst_ref=dst, send_sem=send_sem, recv_sem=recv_sem, device_id=device, device_id_type=MESH
        )
        if when is None:
            copy.start()
        else:
            pl.when(when)(copy.start)
        ends.append((copy, when))

    def arrived(ref, sem):
        pltpu.make_async_copy(ref, ref, sem).wait()

    for b in range(2):
        for m in range(2):
            mine = jnp.logical_and(2 * c + b == y, c == m)
            send(
                pack.at[b, m], w.at[z, y], a_send.at[2 * b + m], a_recv,
                at(ny=2 * c + b, nc=m), jnp.logical_not(mine),
            )

            @pl.when(mine)
            def _():
                w[z, y] = pack[b, m]

    for k, n in enumerate(xs):
        send(tok.at[y, c, x], tok.at[y, c, x], t_send.at[k], tx_recv, at(nx=n))
        send(par.at[c, x], par.at[c, x], p_send.at[k], px_recv, at(nx=n))

    relay = z // 4
    for m in range(2):
        mine = jnp.logical_and(x == relay, c == m)
        spot = ow.at[z % 4, y, :, pl.ds(pl.multiple_of((2 * x + c) * 128, 128), 128)]
        send(opack.at[m], spot, o1_send.at[m], o1_recv, at(nx=relay, nc=m), jnp.logical_not(mine))

        @pl.when(mine)
        def _():
            ow[z % 4, y, :, pl.ds(pl.multiple_of((2 * x + c) * 128, 128), 128)] = opack[m]

    own_piece = (y // 2) == c

    @pl.when(own_piece)
    def _():
        arrived(w.at[z, 0:3], a_recv)

    @pl.when(jnp.logical_not(own_piece))
    def _():
        arrived(w.at[z], a_recv)

    def w_block(d):
        return w.at[lax.rem(z - d + NZ, NZ)]

    def w_index(d):
        return d - 1 if d > 0 else 7 - d

    def w_pass(d, hop):
        block = w_block(d)
        send(block, block, w_send.at[w_index(d + hop)], w_recv.at[w_index(d + hop)], at(dz=hop))

    def o_block(d):
        source = lax.rem(z - d + NZ, NZ)
        return (source // 4) == x, lax.rem(source, 4)

    def o_pass(d, hops):
        here, zi = o_block(d)
        block = ow.at[zi, y]
        if d != 0:
            pl.when(here)(lambda: arrived(block, o2_recv.at[zi]))
        for hop in hops:
            spot = {1: 0, 2: 1, -1: 2, -2: 3}[hop]
            send(block, block, o2_send.at[w_index(d + hop)], o2_recv.at[zi], at(dz=hop), here)
        for k, n in enumerate(ys):
            send(block, block, o3_send.at[8 + d, k], o3_recv, at(ny=n), here)

    for hop in (2, -2, 1, -1):
        w_pass(0, hop)

    @pl.when(x == relay)
    def _():
        arrived(ow.at[z % 4, y, :, 0:896], o1_recv)

    o_pass(0, (2, -2, 1, -1))

    arrived(tok.at[y, c, 0:3], tx_recv)
    for k, n in enumerate(ys):
        send(tok.at[y, c], tok.at[y, c], t_send.at[3 + k], ty_recv.at[k], at(ny=n))
    arrived(par.at[c, 0:3], px_recv)
    send(par.at[c], par.at[c], p_send.at[3], pd_recv, at(nc=other))
    send(tok.at[y, c], tok.at[y, c], t_send.at[6], td_recv, at(nc=other))

    for k in (1, 2, 3):
        for d in (2 * k, -2 * k):
            arrived(w_block(d), w_recv.at[w_index(d)])
            for hop in (2, 1) if d > 0 else ((-2, -1) if k < 3 else (-1,)):
                w_pass(d, hop)
        for d in (2 * k - 1, 1 - 2 * k):
            o_pass(d, ())
        for d in (2 * k, -2 * k):
            o_pass(d, (2, 1) if d > 0 else ((-2, -1) if k < 3 else (-1,)))
        if k == 2:
            for j in range(3):
                rows = tok.at[lax.rem(y - j - 1 + NY, NY), c]
                arrived(rows, ty_recv.at[j])
                send(rows, rows, t_send.at[7 + j], td_recv, at(nc=other))
    arrived(tok.at[:, other], td_recv)
    arrived(par.at[other], pd_recv)

    def normalise(i, _):
        total = jnp.zeros((TOK, 128), F32)
        for m in range(2):
            for n in range(NX):
                v = tok[i, m, n].astype(F32)
                total += v * v
        scale = lax.rsqrt(jnp.sum(total, axis=1, keepdims=True) / 1024 + EPS)
        rows = pl.ds(pl.multiple_of(i * TOK, TOK), TOK)
        for m in range(2):
            for n in range(NX):
                v = tok[i, m, n].astype(F32) * scale * par[m, n, 0:1, :]
                t = 128 * (2 * n + m)
                normed[rows, t : t + 128] = v.astype(BF16)
        return 0

    lax.fori_loop(0, NY, normalise, 0)

    for d in (1, -1, 3, -3, 5, -5, 7, -7, 8):
        arrived(w_block(d), w_recv.at[w_index(d)])

    weights = w[...].reshape(1024, 256)
    half = lanes((TOK, 128)) < 64
    for i in range(NY):
        rows = slice(i * TOK, i * TOK + TOK)
        spot = slice(HALO + i * TOK, HALO + i * TOK + TOK)
        result = jnp.dot(normed[rows, :], weights, preferred_element_type=F32)
        one, two = result[:, :128], result[:, 128:]
        two_b = two.astype(BF16)

        @pl.when(c == 0)
        def _():
            kv[spot, :] = two_b
            qp[rows, :] = jnp.where(half, one, 0.0).astype(BF16)

        @pl.when(c == 1)
        def _():
            mix = one.astype(BF16).astype(F32) * two_b.astype(F32)
            kv[spot, :] = swap(mix).astype(BF16)
            qp[rows, :] = two_b

        gsend[i] = fold(jax.nn.sigmoid(one))

    for k, hop in enumerate((1, -1)):
        src = kv.at[ROWS : ROWS + HALO] if hop == 1 else kv.at[HALO : 2 * HALO]
        dst = kv.at[0:HALO] if hop == 1 else kv.at[ROWS + HALO : ROWS + 2 * HALO]
        send(src, dst, h_send.at[k], h_recv.at[k], at(dz=hop))
    for k, n in enumerate(ys):
        send(gsend.at[n], grecv.at[y], g_send.at[k], g_recv, at(ny=n))
    grecv[y] = gsend[y]

    for d in (7, -7, 8):
        o_pass(d, ())

    small = par[y // 2, x]
    sink_here = jnp.sum(jnp.where(lanes((1, 128)) == lax.rem(y, 2), small[4:5, :], 0.0), axis=1, keepdims=True)
    tap_rows = jnp.where(lax.rem(y, 2) == 1, small, swap(small))

    def attend(i):
        q = qp[i * TOK : i * TOK + TOK, :]
        keys = kv[i * TOK : i * TOK + TOK + 2 * HALO, :]
        s = lax.dot_general(q, keys, (((1,), (1,)), ((), ())), preferred_element_type=F32) * 0.125
        gap = lanes(s.shape) - lax.broadcasted_iota(jnp.int32, s.shape, 0)
        place = z * ROWS + (i * TOK - HALO) + lanes(s.shape)
        allowed = (gap >= 0) & (gap <= 2 * HALO) & (place >= 0) & (place < SEQ)
        s = jnp.where(allowed, s, NEG)
        top = jnp.maximum(jnp.max(s, axis=1, keepdims=True), sink_here)
        p = jnp.exp(s - top)
        total = jnp.sum(p, axis=1, keepdims=True) + jnp.exp(sink_here - top)
        high = p.astype(BF16)
        low = (p - high.astype(F32)).astype(BF16)
        mixed = jnp.dot(high, keys, preferred_element_type=F32) + jnp.dot(low, keys, preferred_element_type=F32)
        asend[i] = fold(mixed / total).astype(BF16)

    def convolve(i):
        wide = kv[HALO - 16 + i * TOK : HALO + 16 + i * TOK + TOK, :].astype(F32)
        size = wide.shape[0]
        before = pltpu.roll(wide, 1, 0)[16 : 16 + TOK]
        after = pltpu.roll(wide, size - 1, 0)[16 : 16 + TOK]
        place = z * ROWS + i * TOK + lax.broadcasted_iota(jnp.int32, before.shape, 0)
        before = jnp.where(place == 0, 0.0, before)
        after = jnp.where(place == SEQ - 1, 0.0, after)
        total = tap_rows[1:2] * before + tap_rows[2:3] * wide[16 : 16 + TOK] + tap_rows[3:4] * after
        asend[i] = fold(qp[i * TOK : i * TOK + TOK, :].astype(F32) * total).astype(BF16)

    for step, i in enumerate((1, 2, 0, 3)):
        if i == 0:
            arrived(kv.at[0:HALO], h_recv.at[0])
        if i == 3:
            arrived(kv.at[ROWS + HALO : ROWS + 2 * HALO], h_recv.at[1])
        pl.when(c == 0)(lambda: attend(i))
        pl.when(c == 1)(lambda: convolve(i))
        for n in range(NX):
            mine = jnp.logical_and(y == i, x == n)
            send(
                asend.at[i], arecv.at[4 * x + y], e_send.at[4 * i + n], e_recv,
                at(ny=i, nx=n), jnp.logical_not(mine),
            )
    arecv[4 * x + y] = asend[y]

    arrived(ow.at[0:3], o3_recv)
    arrived(grecv.at[0:3], g_recv)
    arrived(arecv.at[0:15], e_recv)
    for j in range(8):
        low, high = unfold(arecv[2 * j].astype(F32), arecv[2 * j + 1].astype(F32))
        left[0:64, 128 * j : 128 * j + 128] = low.astype(BF16)
        left[64:128, 128 * j : 128 * j + 128] = high.astype(BF16)
    branch = lax.dot_general(
        left[...], ow[...].reshape(256, 1024), (((1,), (1,)), ((), ())), preferred_element_type=F32
    )
    parts = []
    for j in range(2):
        low, high = unfold(grecv[2 * j], grecv[2 * j + 1])
        parts.append(branch[:, 128 * j : 128 * j + 128] * jnp.concatenate([low, high], axis=0))
    xsend[...] = jnp.where(c == 0, parts[1], parts[0])
    send(xsend, xrecv, d_send, d_recv, at(nc=other))
    kept = jnp.where(c == 0, parts[0], parts[1])
    arrived(xrecv, d_recv)
    out[...] = (kept + xrecv[...]).astype(BF16)

    for copy, when in ends:
        if when is None:
            copy.wait_send()
        else:
            pl.when(when)(copy.wait_send)


def on_device(
    tokens, norm_gain, query_weight, key_weight, value_weight, conv_in_weight, pre_weight, post_weight,
    attn_gate_weight, conv_gate_weight, sink_logit, conv_taps, attn_out_weight, conv_out_weight,
):
    dma = pltpu.SemaphoreType.DMA
    vmem = pltpu.VMEM
    return pl.pallas_call(
        kernel,
        out_shape=jax.ShapeDtypeStruct((TOK, 128), BF16),
        in_specs=[pl.BlockSpec(memory_space=pl.ANY)] * 14,
        out_specs=pl.BlockSpec(memory_space=pltpu.VMEM),
        scratch_shapes=[
            vmem((NY, 2, NX, TOK, 128), BF16),
            vmem((2, NX, 8, 128), F32),
            vmem((NZ, NY, 16, 256), BF16),
            vmem((4, NY, 16, 1024), BF16),
            vmem((ROWS, 1024), BF16),
            vmem((ROWS + 2 * HALO, 128), BF16),
            vmem((ROWS, 128), BF16),
            vmem((NY, 64, 128), F32),
            vmem((NY, 64, 128), F32),
            vmem((NY, 64, 128), BF16),
            vmem((NX * NY, 64, 128), BF16),
            vmem((TOK, 1024), BF16),
            vmem((TOK, 128), F32),
            vmem((TOK, 128), F32),
            vmem((6, 16, 128), BF16),
            vmem((16, 64), BF16),
            vmem((16, 64), BF16),
            vmem((2, 128, 16), BF16),
            vmem((1, 128), F32),
            vmem((3, 128), F32),
            vmem((1, 2), F32),
            vmem((2, 2, 16, 256), BF16),
            vmem((2, 16, 128), BF16),
            dma((14,)),
            dma((4,)), dma,
            dma((10,)), dma, dma((3,)), dma,
            dma((4,)), dma, dma,
            dma((15,)), dma((15,)),
            dma((2,)), dma,
            dma((15,)), dma((4,)),
            dma((17, 3)), dma,
            dma((2,)), dma((2,)),
            dma((3,)), dma,
            dma((16,)), dma,
            dma, dma,
        ],
        compiler_params=pltpu.CompilerParams(collective_id=0, has_side_effects=True, vmem_limit_bytes=48 << 20),
    )(
        tokens, norm_gain.reshape(1, 128), query_weight, key_weight, value_weight, conv_in_weight, pre_weight,
        post_weight, attn_gate_weight, conv_gate_weight, sink_logit.reshape(1, 2), conv_taps, attn_out_weight,
        conv_out_weight,
    )


def solution(mesh):
    fine = Mesh(mesh.devices.reshape(NZ, NY, NX, 2), ("z", "y", "x", "c"))
    sp, tp = ("z", "y"), ("x", "c")
    return jax.shard_map(
        on_device,
        mesh=fine,
        in_specs=(P(sp, tp), P(tp)) + (P(sp, tp),) * 8 + (P(tp), P(None, tp), P(tp, sp), P(tp, sp)),
        out_specs=P(sp, tp),
        check_vma=False,
    )
```
